32 devices in a mesh: ep: 8 (over z, y), tp: 4 (over x, core).
Axes of the slice: x: 2, y: 2, z: 4, core: 2. Of those that a mesh axis runs over, the one named last changes fastest.
Arguments:
- hidden: bfloat16 [32, 2048], P('ep'), may hold values from -6 to 6
- lengths: int32 [32], P(('ep', 'tp')), may hold values from 1 to 1535, 24576 in all
- latent_cache: bfloat16 [32, 1536, 512], P(('ep', 'tp')), may hold values from -6 to 6
- cache_rotary: bfloat16 [32, 32, 1536], P(('ep', 'tp')), may hold values from -1500 to 1500
- attn_gain: bfloat16 [2048], replicated, may hold values from 0.099609375 to 1.8984375
- w_query_nope: bfloat16 [2048, 1024], P(None, 'tp'), may hold values from -0.125 to 0.125
- w_query_rope: bfloat16 [2048, 512], P(None, 'tp'), may hold values from -0.125 to 0.125
- latent_weight: bfloat16 [2048, 512], replicated, may hold values from -0.125 to 0.125
- w_rotary_key: bfloat16 [2048, 32], replicated, may hold values from -0.125 to 0.125
- latent_norm_gain: bfloat16 [512], replicated, may hold values from 0.099609375 to 1.8984375
- key_up_weight: bfloat16 [1024, 512], P('tp'), may hold values from -0.75 to 0.75
- value_up_weight: bfloat16 [512, 1024], P(None, 'tp'), may hold values from -0.25 to 0.25
- head_gain: bfloat16 [1024], P('tp'), may hold values from 0.099609375 to 1.8984375
- w_output: bfloat16 [1024, 2048], P('tp'), may hold values from -0.1875 to 0.1875
- ffn_gain: bfloat16 [2048], replicated, may hold values from 0.099609375 to 1.8984375
- expert_ids: int32 [32, 4], P('ep'), may hold values from 0 to 7, all different within a row; in each aligned block of 4 rows (0 to 3, 4 to 7, ...) at most 3 rows name the same one
- expert_weights: float32 [32, 4], P('ep'), may hold values from 0.2 to 1.2
- w_expert_gate: bfloat16 [8, 2048, 2048], P('ep', None, 'tp'), may hold values from -0.125 to 0.125
- w_expert_up: bfloat16 [8, 2048, 2048], P('ep', None, 'tp'), may hold values from -0.125 to 0.125
- w_expert_down: bfloat16 [8, 2048, 2048], P('ep', 'tp'), may hold values from -0.125 to 0.125
- w_shared_gate: bfloat16 [2048, 1024], P(None, 'tp'), may hold values from -0.125 to 0.125
- w_shared_up: bfloat16 [2048, 1024], P(None, 'tp'), may hold values from -0.125 to 0.125
- w_shared_down: bfloat16 [1024, 2048], P('tp'), may hold values from -0.1875 to 0.1875
- w_dense_up: bfloat16 [2048, 2048], P(None, 'tp'), may hold values from -0.125 to 0.125
- w_dense_down: bfloat16 [2048, 2048], P('tp'), may hold values from -0.125 to 0.125
- dense_gate: bfloat16 [2048], replicated, may hold values from -0.125 to 0.125
Outputs:
- layer_out: bfloat16 [32, 2048], P('ep', 'tp')
The draws below stay inside these ranges and needn't reach their ends.
Inputs may be any that keep to these rules, and one draw needn't show every extreme that they name: `lengths`: past positions of each sequence; the longest has exactly 1535, so every cache has room for the new token. `expert_ids`: A row's 4 experts differ. Among the rows of one index of ep (4 rows), no expert is named by more than 3 of them, a bound that some block reaches.
All inputs are finite; a program needn't handle non-finite values. No bound on the sum of `lengths` on one device may be relied on, other than what follows from the above.
Results may differ from the reference program's by a relative error of at most 0.024.
Values may be sent and summed in bfloat16 or wider, within the bound.
A program may use at most 64 MiB of HBM per device.

```python
import math
import jax
import jax.numpy as jnp
import numpy as np
from jax import lax

MODEL_WIDTH = 2048
HEAD_COUNT = 16
PLAIN_QUERY = 64
ROPE = 32
VALUE_UNITS = 64
LATENT_UNITS = 512
E_FF = 2048
S_FF = 1024
DENSE_FF = 2048
TOPK = 4
CACHE_LENGTH = 1536
SEQ_GRP = 4
SEQUENCE_COUNT = 32
EXPERTS = 8
CAP = 3
N_EP = 8
N_TP = 4


def draw_cache_rotary(key, part):
    base_key = jax.random.fold_in(key, 11)
    values = jnp.clip(jax.random.normal(base_key, (SEQUENCE_COUNT, ROPE, CACHE_LENGTH), jnp.float32), -6.0, 6.0)
    return values.astype(jnp.bfloat16)


def shard_levels(key, extent, pieces, smallest, top_value):
    def one(position, parts):
        heights = jax.random.uniform(jax.random.fold_in(jax.random.fold_in(key, 6), position), (parts,), jnp.float32, smallest / len(pieces), top_value / len(pieces))
        return jnp.repeat(jnp.exp(heights), extent[position] // parts).reshape((-1,) + (1,) * (len(extent) - position - 1))

    factor_of = one(*pieces[0])
    for cut in pieces[1:]:
        factor_of = factor_of * one(*cut)
    return factor_of


def split_up(count, total, limit, lean):
    portions = [(1 << 20) // math.isqrt(grade ** lean) + 1 for grade in range(2, count + 1)]
    spare, counts = total - limit - (count - 1), [1] * (count - 1)
    while spare > 0:
        candidates = [i for i in range(count - 1) if counts[i] < limit]
        whole, left = sum([portions[i] for i in candidates]), spare
        for i in candidates:
            addition = min(limit - counts[i], max(1, left * portions[i] // whole), spare)
            counts[i] = counts[i] + addition
            spare = spare - addition
    return np.array([limit] + counts)


def ragged_sizes(key, count, total, bound, slope):
    if count == 2:
        one = jax.random.randint(key, (), max(1, total - bound), min(bound, total - 1) + 1)
        return jnp.stack([one, total - one])
    sizes = jnp.asarray(split_up(count, total, bound, slope), jnp.int32)
    pairs = (count - 1) // 2
    source_of, receiver = sizes[1:1 + 2 * pairs:2], sizes[2:2 + 2 * pairs:2]
    slack = jnp.minimum(source_of - 1, bound - receiver)
    shifted = jax.random.randint(jax.random.fold_in(key, 1), (pairs,), 0, 1 << 20) % (slack + 1)
    sizes = sizes.at[1:1 + 2 * pairs:2].set(source_of - shifted).at[2:2 + 2 * pairs:2].set(receiver + shifted)
    return sizes[jax.random.permutation(jax.random.fold_in(key, 2), count)]


def deal_out(rng, own, number, rows, count, top, limit, skew):
    ranking = jax.random.permutation(rng, count)
    heavy_load, ordinary = load_shares(count, rows * top, limit, skew, True), load_shares(count, rows * top, limit, skew, False)
    places = jnp.arange(count)

    def named(sizes, rotation):
        used = int((sizes > 0).sum())
        fixed = max(1, used // 4)
        passed = fixed + (places - fixed + rotation * (used - fixed)) % max(1, count - fixed)
        return jnp.zeros((count,), jnp.int32).at[ranking[jnp.where(places < fixed, places, passed)]].set(jnp.asarray(sizes, jnp.int32))

    sizes = jnp.where(number % 4 == 0, named(heavy_load, number // 4), named(ordinary, number - number // 4 - 1))
    mixed = jax.random.permutation(jax.random.fold_in(own, 3), count)
    source_of, receiver = mixed[0:count // 2 * 2:2], mixed[1:count // 2 * 2:2]
    slack = jnp.minimum(sizes[source_of] - 1, limit - sizes[receiver]) // 2
    slack = jnp.where((source_of == ranking[0]) | (receiver == ranking[0]) | (sizes[receiver] == 0), 0, jnp.maximum(slack, 0))
    passed = jax.random.randint(jax.random.fold_in(own, 4), (count // 2,), 0, 1 << 20) % (slack + 1)
    sizes = sizes.at[source_of].add(-passed).at[receiver].add(passed)
    items = jnp.searchsorted(jnp.cumsum(sizes), jnp.arange(rows * top), side="right").astype(jnp.int32)
    listing = items.reshape(top, rows).T
    listing = listing[jax.random.permutation(jax.random.fold_in(own, 1), rows)]
    rotation = jax.random.randint(jax.random.fold_in(own, 2), (rows, 1), 0, top)
    return jnp.take_along_axis(listing, (jnp.arange(top)[None, :] + rotation) % top, axis=1)


def load_shares(number_of, total, bound, skew, full):
    loads = [(1 << 20) // math.isqrt(standing ** skew) + 1 for standing in range(1, number_of + 1)]
    largest = bound if full else min(bound, max(-(-total // number_of), total * loads[0] // sum(loads)))
    least = 1 if total - largest >= number_of - 1 else 0
    counts, surplus = [largest] + [least] * (number_of - 1), total - largest - least * (number_of - 1)
    while surplus > 0:
        candidates = [i for i in range(1, number_of) if counts[i] < largest] or [i for i in range(1, number_of) if counts[i] < bound]
        mass, left = sum([loads[i] for i in candidates]), surplus
        for i in candidates:
            extra = min(bound - counts[i], max(1, left * loads[i] // mass), surplus)
            counts[i] = counts[i] + extra
            surplus = surplus - extra
    return np.array(counts)


def bell_draw(key, extent, deviation, bound, cuts=(), kind=jnp.bfloat16):
    values = deviation * jax.random.normal(key, extent, jnp.float32)
    if cuts:
        values = values * shard_levels(key, extent, cuts, -0.22, 0.18)
    return jnp.clip(values, -bound, bound).astype(kind)


def setup_inputs(seed: int = 0) -> dict:
    arg_keys = jax.random.split(jax.random.key(seed), 27)
    hidden = bell_draw(arg_keys[0], (SEQUENCE_COUNT, MODEL_WIDTH), 1.0, 6.0, ((0, 8),))
    lengths = ragged_sizes(arg_keys[1], SEQUENCE_COUNT, SEQUENCE_COUNT * CACHE_LENGTH // 2, CACHE_LENGTH - 1, 2).astype(jnp.int32)
    latent_cache = bell_draw(arg_keys[2], (SEQUENCE_COUNT, CACHE_LENGTH, LATENT_UNITS), 1.0, 6.0, ((0, 32),))
    cache_rotary = draw_cache_rotary(jax.random.fold_in(arg_keys[26], 71), 0)
    attn_gain = jnp.clip(1.0 + 0.18 * jax.random.normal(arg_keys[4], (MODEL_WIDTH,), jnp.float32), 0.099609375, 1.8984375).astype(jnp.bfloat16)
    w_query_nope = bell_draw(arg_keys[5], (MODEL_WIDTH, HEAD_COUNT * PLAIN_QUERY), MODEL_WIDTH ** -0.5, 0.125, ((1, 4),))
    w_query_rope = bell_draw(arg_keys[6], (MODEL_WIDTH, HEAD_COUNT * ROPE), MODEL_WIDTH ** -0.5, 0.125, ((1, 4),))
    latent_weight = bell_draw(arg_keys[7], (MODEL_WIDTH, LATENT_UNITS), MODEL_WIDTH ** -0.5, 0.125)
    w_rotary_key = bell_draw(arg_keys[8], (MODEL_WIDTH, ROPE), MODEL_WIDTH ** -0.5, 0.125)
    latent_norm_gain = jnp.clip(1.0 + 0.18 * jax.random.normal(arg_keys[9], (LATENT_UNITS,), jnp.float32), 0.099609375, 1.8984375).astype(jnp.bfloat16)
    key_up_weight = bell_draw(arg_keys[10], (HEAD_COUNT * PLAIN_QUERY, LATENT_UNITS), PLAIN_QUERY ** -0.5, 0.75, ((0, 4),))
    value_up_weight = bell_draw(arg_keys[11], (LATENT_UNITS, HEAD_COUNT * VALUE_UNITS), LATENT_UNITS ** -0.5, 0.25, ((1, 4),))
    head_gain = jnp.clip(1.0 + 0.18 * jax.random.normal(arg_keys[12], (HEAD_COUNT * VALUE_UNITS,), jnp.float32), 0.099609375, 1.8984375).astype(jnp.bfloat16)
    w_output = bell_draw(arg_keys[13], (HEAD_COUNT * VALUE_UNITS, MODEL_WIDTH), (HEAD_COUNT * VALUE_UNITS) ** -0.5, 0.1875, ((0, 4),))
    ffn_gain = jnp.clip(1.0 + 0.18 * jax.random.normal(arg_keys[14], (MODEL_WIDTH,), jnp.float32), 0.099609375, 1.8984375).astype(jnp.bfloat16)
    expert_ids_keys = jax.random.split(jax.random.fold_in(arg_keys[15], 1), SEQUENCE_COUNT // SEQ_GRP)
    expert_ids_turns = jax.random.permutation(jax.random.fold_in(arg_keys[15], 3), SEQUENCE_COUNT // SEQ_GRP)
    expert_ids = jax.vmap(lambda own, number: deal_out(jax.random.fold_in(arg_keys[15], 2), own, number, SEQ_GRP, EXPERTS, TOPK, CAP, 2))(expert_ids_keys, expert_ids_turns).reshape((SEQUENCE_COUNT, TOPK))
    expert_weights = jnp.clip(0.2 + 1 * jax.random.uniform(arg_keys[16], (SEQUENCE_COUNT, TOPK), jnp.float32) ** shard_levels(arg_keys[16], (SEQUENCE_COUNT, TOPK), ((0, 8),), -0.2, 0.2), 0.2, 1.2)
    w_expert_gate = bell_draw(arg_keys[17], (EXPERTS, MODEL_WIDTH, E_FF), MODEL_WIDTH ** -0.5, 0.125, ((0, 8), (2, 4)))
    w_expert_up = bell_draw(arg_keys[18], (EXPERTS, MODEL_WIDTH, E_FF), MODEL_WIDTH ** -0.5, 0.125, ((0, 8), (2, 4)))
    w_expert_down = bell_draw(arg_keys[19], (EXPERTS, E_FF, MODEL_WIDTH), E_FF ** -0.5, 0.125, ((0, 8), (1, 4)))
    w_shared_gate = bell_draw(arg_keys[20], (MODEL_WIDTH, S_FF), MODEL_WIDTH ** -0.5, 0.125, ((1, 4),))
    w_shared_up = bell_draw(arg_keys[21], (MODEL_WIDTH, S_FF), MODEL_WIDTH ** -0.5, 0.125, ((1, 4),))
    w_shared_down = bell_draw(arg_keys[22], (S_FF, MODEL_WIDTH), S_FF ** -0.5, 0.1875, ((0, 4),))
    w_dense_up = bell_draw(arg_keys[23], (MODEL_WIDTH, DENSE_FF), MODEL_WIDTH ** -0.5, 0.125, ((1, 4),))
    w_dense_down = bell_draw(arg_keys[24], (DENSE_FF, MODEL_WIDTH), DENSE_FF ** -0.5, 0.125, ((0, 4),))
    dense_gate = bell_draw(arg_keys[25], (MODEL_WIDTH,), MODEL_WIDTH ** -0.5, 0.125)
    return {"hidden": hidden, "lengths": lengths, "latent_cache": latent_cache, "cache_rotary": cache_rotary, "attn_gain": attn_gain, "w_query_nope": w_query_nope, "w_query_rope": w_query_rope, "latent_weight": latent_weight, "w_rotary_key": w_rotary_key, "latent_norm_gain": latent_norm_gain, "key_up_weight": key_up_weight, "value_up_weight": value_up_weight, "head_gain": head_gain, "w_output": w_output, "ffn_gain": ffn_gain, "expert_ids": expert_ids, "expert_weights": expert_weights, "w_expert_gate": w_expert_gate, "w_expert_up": w_expert_up, "w_expert_down": w_expert_down, "w_shared_gate": w_shared_gate, "w_shared_up": w_shared_up, "w_shared_down": w_shared_down, "w_dense_up": w_dense_up, "w_dense_down": w_dense_down, "dense_gate": dense_gate}


def norm_rows(values, gains):
    values = values.astype(jnp.float32)
    factor = lax.rsqrt(lax.optimization_barrier(jnp.mean(values * values, axis=-1, keepdims=True)) + 1e-06)
    return values * factor * gains.astype(jnp.float32)

def angles_at(positions, rot_width):
    half_width = rot_width // 2
    inverse = 1.0 / 10000.0 ** (jnp.arange(half_width, dtype=jnp.float32) / half_width)
    return positions.astype(jnp.float32)[..., None] * inverse

def rotate(values, angles):
    half_width = values.shape[-1] // 2
    first = values[..., :half_width]
    second = values[..., half_width:]
    cosines = jnp.cos(angles)
    sines = jnp.sin(angles)
    return jnp.concatenate([first * cosines - second * sines, first * sines + second * cosines], axis=-1)

def block_sum(act_values, down_weight):
    shares = jnp.einsum('rnf,nfd->rnd', act_values.astype(jnp.float32).reshape(act_values.shape[0], N_TP, -1), down_weight.astype(jnp.float32).reshape(N_TP, -1, MODEL_WIDTH))
    return lax.optimization_barrier(jnp.sum(lax.optimization_barrier(shares.astype(jnp.bfloat16)).astype(jnp.float32), axis=1))

def reference(hidden, lengths, latent_cache, cache_rotary, attn_gain, w_query_nope, w_query_rope, latent_weight, w_rotary_key, latent_norm_gain, key_up_weight, value_up_weight, head_gain, w_output, ffn_gain, expert_ids, expert_weights, w_expert_gate, w_expert_up, w_expert_down, w_shared_gate, w_shared_up, w_shared_down, w_dense_up, w_dense_down, dense_gate):
    normed = norm_rows(hidden, attn_gain).astype(jnp.bfloat16)
    query_unrotated = jnp.dot(normed, w_query_nope, preferred_element_type=jnp.float32).astype(jnp.bfloat16)
    query_unrotated = query_unrotated.reshape(SEQUENCE_COUNT, HEAD_COUNT, PLAIN_QUERY)
    query_rope = jnp.dot(normed, w_query_rope, preferred_element_type=jnp.float32).astype(jnp.bfloat16)
    query_rope = query_rope.reshape(SEQUENCE_COUNT, HEAD_COUNT, ROPE)
    query_in_latent = jnp.einsum('tba,bai->tbi', query_unrotated.astype(jnp.float32), key_up_weight.reshape(HEAD_COUNT, PLAIN_QUERY, LATENT_UNITS).astype(jnp.float32)).astype(jnp.bfloat16)
    angles = angles_at(lengths, ROPE)
    query_rotated = rotate(query_rope.astype(jnp.float32), angles[:, None, :]).astype(jnp.bfloat16)
    new_latent = norm_rows(jnp.dot(normed, latent_weight, preferred_element_type=jnp.float32), latent_norm_gain).astype(jnp.bfloat16)
    new_key = rotate(jnp.dot(normed, w_rotary_key, preferred_element_type=jnp.float32), angles).astype(jnp.bfloat16)
    score_scale = (PLAIN_QUERY + ROPE) ** (-0.5)

    def attend_one(inputs):
        latent_query_rows, rot_query, latents, rot_keys, seq_length, own_latent, own_key = inputs
        latent_query_rows = latent_query_rows.astype(jnp.float32)
        rot_query = rot_query.astype(jnp.float32)
        cache_scores = (jnp.dot(latent_query_rows, latents.astype(jnp.float32).T) + jnp.dot(rot_query, rot_keys.astype(jnp.float32))) * score_scale
        own_scores = (jnp.dot(latent_query_rows, own_latent.astype(jnp.float32)) + jnp.dot(rot_query, own_key.astype(jnp.float32))) * score_scale
        in_cache = jnp.arange(CACHE_LENGTH, dtype=jnp.int32) < seq_length
        cache_scores = jnp.where(in_cache[None, :], cache_scores, -jnp.inf)
        peak = jnp.maximum(lax.optimization_barrier(jnp.max(cache_scores, axis=-1)), own_scores)
        cache_exp = jnp.exp(cache_scores - peak[:, None])
        own_exp = jnp.exp(own_scores - peak)
        weight_sum = lax.optimization_barrier(jnp.sum(cache_exp, axis=-1)) + own_exp
        cache_probs = (cache_exp / weight_sum[:, None]).astype(jnp.bfloat16)
        own_probs = (own_exp / weight_sum).astype(jnp.bfloat16)
        mixed_output = jnp.dot(cache_probs.astype(jnp.float32), latents.astype(jnp.float32))
        mixed_output = mixed_output + own_probs.astype(jnp.float32)[:, None] * own_latent.astype(jnp.float32)[None, :]
        return mixed_output.astype(jnp.bfloat16)
    attended_value = lax.map(attend_one, (query_in_latent, query_rotated, latent_cache, cache_rotary, lengths, new_latent, new_key))
    head_output = jnp.einsum('bqc,cqp->bqp', attended_value.astype(jnp.float32), value_up_weight.reshape(LATENT_UNITS, HEAD_COUNT, VALUE_UNITS).astype(jnp.float32))
    head_output = norm_rows(head_output, head_gain.reshape(HEAD_COUNT, VALUE_UNITS)).astype(jnp.bfloat16).reshape(SEQUENCE_COUNT, HEAD_COUNT * VALUE_UNITS)
    attention = jnp.dot(head_output, w_output, preferred_element_type=jnp.float32)
    middle = (hidden.astype(jnp.float32) + attention).astype(jnp.bfloat16)
    normed_ffn = norm_rows(middle, ffn_gain).astype(jnp.bfloat16)
    group_ids = expert_ids.reshape(N_EP, SEQ_GRP * TOPK)
    matches = (group_ids[:, :, None] == jnp.arange(EXPERTS, dtype=jnp.int32)[None, None, :]).astype(jnp.int32)
    slot_index = lax.optimization_barrier(jnp.sum((jnp.cumsum(matches, axis=1) - matches) * matches, axis=2))
    target = (group_ids * CAP + slot_index).reshape(N_EP, SEQ_GRP, TOPK)
    places = jnp.arange(EXPERTS * CAP, dtype=jnp.int32)
    chosen = places[None, :, None, None] == target[:, None, :, :]
    dispatch = jnp.any(chosen, axis=3).astype(jnp.float32)
    grouped_rows = normed_ffn.reshape(N_EP, SEQ_GRP, MODEL_WIDTH).astype(jnp.float32)
    sent_rows = jnp.einsum('gcs,gsd->gcd', dispatch, grouped_rows).astype(jnp.bfloat16)
    sent_rows = jnp.swapaxes(sent_rows.reshape(N_EP, EXPERTS, CAP, MODEL_WIDTH), 0, 1).reshape(EXPERTS, N_EP * CAP, MODEL_WIDTH)

    def run_expert(inputs):
        expert_rows, gate_weight, up_weight, down_weight = inputs
        expert_rows = expert_rows.astype(jnp.float32)
        gate_pre = jnp.dot(expert_rows, gate_weight.astype(jnp.float32))
        up_pre = jnp.dot(expert_rows, up_weight.astype(jnp.float32))
        act_values = (jax.nn.silu(gate_pre) * up_pre).astype(jnp.bfloat16)
        return block_sum(act_values, down_weight).astype(jnp.bfloat16)
    slot_out = lax.map(run_expert, (sent_rows, w_expert_gate, w_expert_up, w_expert_down))
    slot_out = jnp.swapaxes(slot_out.reshape(EXPERTS, N_EP, CAP, MODEL_WIDTH), 0, 1).reshape(N_EP, EXPERTS * CAP, MODEL_WIDTH)
    group_weights = expert_weights.reshape(N_EP, SEQ_GRP, TOPK)
    combine = lax.optimization_barrier(jnp.sum(jnp.where(jnp.swapaxes(chosen, 1, 2), group_weights[:, :, None, :], 0.0), axis=3))
    routed = jnp.einsum('gsc,gcd->gsd', combine, slot_out.astype(jnp.float32), precision=lax.Precision.HIGHEST).reshape(SEQUENCE_COUNT, MODEL_WIDTH)
    shared_act = (jax.nn.silu(jnp.dot(normed_ffn, w_shared_gate, preferred_element_type=jnp.float32)) * jnp.dot(normed_ffn, w_shared_up, preferred_element_type=jnp.float32)).astype(jnp.bfloat16)
    dense_act = jax.nn.gelu(jnp.dot(normed_ffn, w_dense_up, preferred_element_type=jnp.float32)).astype(jnp.bfloat16)
    mix_gate = jax.nn.sigmoid(jnp.dot(normed_ffn, dense_gate, preferred_element_type=jnp.float32))
    shared_shares = jnp.einsum('rnf,nfd->rnd', shared_act.astype(jnp.float32).reshape(SEQUENCE_COUNT, N_TP, -1), w_shared_down.astype(jnp.float32).reshape(N_TP, -1, MODEL_WIDTH))
    dense_shares = jnp.einsum('rnf,nfd->rnd', dense_act.astype(jnp.float32).reshape(SEQUENCE_COUNT, N_TP, -1), w_dense_down.astype(jnp.float32).reshape(N_TP, -1, MODEL_WIDTH))
    side_terms = shared_shares + mix_gate[:, None, None] * dense_shares
    side = lax.optimization_barrier(jnp.sum(lax.optimization_barrier(side_terms.astype(jnp.bfloat16)).astype(jnp.float32), axis=1))
    return (middle.astype(jnp.float32) + routed + side).astype(jnp.bfloat16)
```

```python
import functools
import math
from typing import Any, NamedTuple

import jax
import jax.numpy as jnp
import numpy as np
from jax import lax
from jax.experimental import pallas as pl
from jax.experimental.pallas import tpu as pltpu
from jax.sharding import PartitionSpec as P

PLAIN_QUERY = 64
ROPE = 32
EPS = 1e-06
F32 = jnp.float32
BF16 = jnp.bfloat16
MESH = pl.DeviceIdType.MESH
VMEM = pltpu.VMEM

class Arrays(NamedTuple):
    hidden: Any
    attn_gain: Any
    w_query_nope: Any
    w_query_rope: Any
    key_up_weight: Any
    latent_norm_gain: Any
    w_rotary_key: Any
    latent_weight: Any
    cache_rotary: Any
    latent_cache: Any
    value_up_weight: Any
    head_gain: Any
    w_output: Any
    ffn_gain: Any
    dense_gate: Any
    expert_ids: Any
    expert_weights: Any
    w_shared_gate: Any
    w_shared_up: Any
    w_dense_up: Any
    w_shared_down: Any
    w_dense_down: Any
    w_expert_gate: Any
    w_expert_up: Any
    w_expert_down: Any


def dot(a, b):
    return jnp.dot(a, b, preferred_element_type=F32)


def dot_t(a, b):
    return lax.dot_general(a, b, (((1,), (1,)), ((), ())), preferred_element_type=F32)


def as_row(ref):
    return ref[...].astype(F32).reshape(1, -1)


def norm_factor(values):
    return lax.rsqrt(jnp.mean(values * values, axis=-1, keepdims=True) + EPS)


def rounded(values):
    return values.astype(BF16).astype(F32)


def stack(ref, count):
    return jnp.concatenate([ref[i].astype(F32) for i in range(count)], axis=0)


def far_first(count):
    return sorted(range(1, count), key=lambda d: -min(d, count - d))


def meet_rounds(count):
    return max(2, (count - 2).bit_length())


def iota(shape, dim):
    return lax.broadcasted_iota(jnp.int32, shape, dim)


def half_turn(values):
    half = values.shape[-1] // 2
    return jnp.concatenate([values[:, half:], values[:, :half]], axis=1)


def layer_kernel(n_ep, n_tp, *refs):
    count = len(Arrays._fields)
    lengths_hbm = refs[0]
    hbm = refs[1 : 1 + count]
    out_ref = refs[1 + count]
    vm = refs[2 + count : 2 + 2 * count]
    (
        lengths_ref,
        fetch_sem,
        q_send,
        q_recv,
        a_send,
        a_recv,
        p_buf,
        mid_buf,
        x_buf,
        s_send,
        s_recv,
        e_send,
        e_recv,
        r_send,
        r_recv,
        tp_sems,
        ep_sems,
        meet_sems,
    ) = refs[2 + 2 * count :]
    ep = lax.axis_index("ep")
    tp = lax.axis_index("tp")

    fetches = [
        pltpu.make_async_copy(source, target, fetch_sem.at[i])
        for i, (source, target) in enumerate(zip(hbm, vm))
    ]
    place = Arrays(*range(count))
    fetch_lengths = pltpu.make_async_copy(lengths_hbm, lengths_ref, fetch_sem.at[count])

    def begin(first, last):
        for fetch in fetches[first : last + 1]:
            fetch.start()

    begin(place.hidden, place.key_up_weight)
    fetch_lengths.start()

    def loader(fetch, ref):
        def load():
            fetch.wait()
            return ref

        return load

    load = Arrays(*map(loader, fetches, vm))

    def tp_peer(d):
        return lax.rem(tp + d, n_tp)

    def ep_peer(d):
        return lax.rem(ep + d, n_ep)

    barrier = pltpu.get_barrier_semaphore()
    for d in range(1, n_tp):
        pl.semaphore_signal(barrier, inc=1, device_id=(ep, tp_peer(d)), device_id_type=MESH)

    def greet(semaphores, reach):
        for side, step in enumerate((reach, -reach)):

            @pl.when((ep + step >= 0) & (ep + step < n_ep))
            def _():
                pl.semaphore_signal(
                    semaphores[side], inc=1, device_id=(ep + step, tp), device_id_type=MESH
                )

    def greeted(semaphores, reach):
        for side, step in enumerate((-reach, reach)):

            @pl.when((ep + step >= 0) & (ep + step < n_ep))
            def _():
                pl.semaphore_wait(semaphores[side], 1)

    reaches = [2**r for r in range(meet_rounds(n_ep))]

    def meet(r):
        return [meet_sems.at[r % len(reaches), side] for side in range(2)]

    greet([barrier, barrier], 1)

    def tp_copy(phase, d, src, dst, to):
        return pltpu.make_async_remote_copy(
            src_ref=src,
            dst_ref=dst,
            send_sem=tp_sems.at[phase, 0, d],
            recv_sem=tp_sems.at[phase, 1, d],
            device_id=(ep, to),
            device_id_type=MESH,
        )

    def ep_copy(phase, d, src, dst, to):
        return pltpu.make_async_remote_copy(
            src_ref=src,
            dst_ref=dst,
            send_sem=ep_sems.at[phase, 0, d],
            recv_sem=ep_sems.at[phase, 1, d],
            device_id=(to, tp),
            device_id_type=MESH,
        )

    started = []

    def go(copy):
        copy.start()
        started.append(copy)
        return copy

    hidden = load.hidden()[...].astype(F32)
    rows, width = hidden.shape
    gain = as_row(load.attn_gain())
    normed = (hidden * norm_factor(hidden) * gain).astype(BF16)
    w_query_nope = load.w_query_nope()
    w_query_rope = load.w_query_rope()
    begin(place.latent_norm_gain, place.latent_cache)
    q_nope = rounded(dot(normed, w_query_nope[...]))
    q_rope = rounded(dot(normed, w_query_rope[...]))
    heads = q_nope.shape[1] // PLAIN_QUERY
    latent = Arrays(*vm).latent_cache.shape[1]

    def by_head(values, unit):
        wide = jnp.concatenate(
            [jnp.broadcast_to(values[i : i + 1], (heads, values.shape[1])) for i in range(rows)],
            axis=0,
        )
        head = iota(wide.shape, 0) % heads
        return jnp.where(iota(wide.shape, 1) // unit == head, wide, 0.0).astype(BF16)

    q_latent = dot(by_head(q_nope, PLAIN_QUERY), load.key_up_weight()[...])
    rope_cols = q_rope.shape[1]
    pick = (iota((rope_cols, ROPE), 0) % ROPE == iota((rope_cols, ROPE), 1)).astype(F32)
    q_rot = dot(by_head(q_rope, ROPE), pick.astype(BF16))
    for i in range(rows):
        part = slice(i * heads, (i + 1) * heads)
        q_send[i, :, :latent] = q_latent[part].astype(q_send.dtype)
        q_send[i, :, latent : latent + ROPE] = q_rot[part].astype(q_send.dtype)
    beside = jnp.where(ep > 0, 1, 0) + jnp.where(ep < n_ep - 1, 1, 0)
    pl.semaphore_wait(barrier, n_tp - 1 + beside)
    greet(meet(0), reaches[0])
    for d in far_first(n_tp):
        go(tp_copy(0, d, q_send.at[tp_peer(d)], q_recv.at[tp], tp_peer(d)))
    q_recv[tp] = q_send[tp]

    own = iota((rows, 1), 0) == tp
    raw_key = dot_t(normed, load.w_rotary_key()[...])
    raw_key = jnp.sum(jnp.where(own, raw_key, 0.0), axis=0, keepdims=True)
    raw_latent = dot(normed, load.latent_weight()[...])
    raw_latent = jnp.sum(jnp.where(own, raw_latent, 0.0), axis=0, keepdims=True)
    latent_gain = as_row(load.latent_norm_gain())
    new_latent = rounded(raw_latent * norm_factor(raw_latent) * latent_gain)
    fetch_lengths.wait()
    length = lengths_ref[...].reshape(1, 1)
    unit = iota((1, ROPE), 1)
    half = ROPE // 2
    inverse = jnp.zeros((1, ROPE), F32)
    for j in range(half):
        inverse = jnp.where(unit % half == j, np.float32(10000.0 ** (-j / half)).item(), inverse)
    angles = length.astype(F32) * inverse
    cosines = jnp.cos(angles)
    sines = jnp.where(unit < half, -1.0, 1.0) * jnp.sin(angles)
    new_key = rounded(raw_key * cosines + half_turn(raw_key) * sines)
    rotary = load.cache_rotary()[...]
    cache_ref = load.latent_cache()
    begin(place.value_up_weight, place.w_expert_down)

    greeted(meet(0), reaches[0])
    greet(meet(1), reaches[1])
    for d in range(1, n_tp):
        started[d - 1].wait_recv()
    query = stack(q_recv, n_tp)
    q_lat = query[:, :latent]
    v = query[:, latent : latent + ROPE]
    q_rotated = rounded(v * cosines + half_turn(v) * sines)
    scale = (PLAIN_QUERY + ROPE) ** (-0.5)
    scores = dot_t(q_lat.astype(BF16), cache_ref[...])
    scores = scores + dot(q_rotated.astype(BF16), rotary)
    scores = jnp.where(iota(scores.shape, 1) < length, scores * scale, -jnp.inf)
    own_score = jnp.sum(q_lat * new_latent, axis=1, keepdims=True)
    own_score = (own_score + jnp.sum(q_rotated * new_key, axis=1, keepdims=True)) * scale
    peak = jnp.maximum(jnp.max(scores, axis=1, keepdims=True), own_score)
    exps = jnp.exp(scores - peak)
    own_exp = jnp.exp(own_score - peak)
    total = jnp.sum(exps, axis=1, keepdims=True) + own_exp
    probs = (exps / total).astype(BF16)
    own_prob = rounded(own_exp / total)
    attended = dot(probs, cache_ref[...]) + own_prob * new_latent
    for t in range(n_tp):
        a_send[t] = attended[t * heads : (t + 1) * heads].astype(a_send.dtype)
    back = [
        go(tp_copy(1, d, a_send.at[tp_peer(d)], a_recv.at[tp], tp_peer(d))) for d in far_first(n_tp)
    ]
    a_recv[tp] = a_send[tp]

    value_up = load.value_up_weight()[...]
    head_gain = as_row(load.head_gain())
    w_output = load.w_output()
    for r in range(1, len(reaches) - 1):
        greeted(meet(r), reaches[r])
        greet(meet(r + 1), reaches[r + 1])
    for copy in back:
        copy.wait_recv()
    values = dot(stack(a_recv, n_tp).astype(BF16), value_up)
    value_units = values.shape[1] // heads
    mine = iota(values.shape, 1) // value_units == iota(values.shape, 0) % heads
    values = jnp.where(mine, values, 0.0)
    mean = jnp.sum(values * values, axis=1, keepdims=True) / value_units
    values = values * lax.rsqrt(mean + EPS)
    values = jnp.concatenate(
        [
            jnp.sum(values[i * heads : (i + 1) * heads], axis=0, keepdims=True)
            for i in range(rows)
        ],
        axis=0,
    )
    head_out = (values * head_gain).astype(BF16)
    p_buf[tp] = dot(head_out, w_output[...]).astype(BF16)
    shares = [go(tp_copy(2, d, p_buf.at[tp], p_buf.at[tp], tp_peer(d))) for d in far_first(n_tp)]
    ffn_gain = as_row(load.ffn_gain())
    gate_vector = as_row(load.dense_gate())
    greeted(meet(-1), reaches[-1])
    for copy in shares:
        copy.wait_recv()
    attention = p_buf[0].astype(F32)
    for t in range(1, n_tp):
        attention = attention + p_buf[t].astype(F32)
    middle = rounded(hidden + attention)
    cols = width // n_tp
    normed_ffn = (middle * norm_factor(middle) * ffn_gain).astype(BF16)
    x_buf[ep] = normed_ffn
    gathers = [go(ep_copy(0, d, x_buf.at[ep], x_buf.at[ep], ep_peer(d))) for d in far_first(n_ep)]

    for t in range(n_tp):
        mid_buf[t] = middle[:, t * cols : (t + 1) * cols]
    gate_pre = dot(normed_ffn, load.w_shared_gate()[...])
    up_pre = dot(normed_ffn, load.w_shared_up()[...])
    shared_act = (gate_pre / (1.0 + jnp.exp(-gate_pre)) * up_pre).astype(BF16)
    pre = dot(normed_ffn, load.w_dense_up()[...])
    inner = math.sqrt(2.0 / math.pi) * (pre + 0.044715 * (pre * pre * pre))
    dense_act = (0.5 * pre * (1.0 + jnp.tanh(inner))).astype(BF16)
    mix = jnp.sum(normed_ffn.astype(F32) * gate_vector, axis=1, keepdims=True)
    mix = 1.0 / (1.0 + jnp.exp(-mix))
    side = dot(shared_act, load.w_shared_down()[...])
    side = side + mix * dot(dense_act, load.w_dense_down()[...])
    for t in range(n_tp):
        s_send[t] = side[:, t * cols : (t + 1) * cols].astype(BF16)
    sides = [
        go(tp_copy(3, d, s_send.at[tp_peer(d)], s_recv.at[tp], tp_peer(d))) for d in far_first(n_tp)
    ]
    s_recv[tp] = s_send[tp]

    w_gate = load.w_expert_gate()
    w_up = load.w_expert_up()
    w_down = load.w_expert_down()
    for copy in gathers:
        copy.wait_recv()
    arrived = stack(x_buf, n_ep).astype(BF16)
    gate_pre = dot(arrived, w_gate[0])
    up_pre = dot(arrived, w_up[0])
    act = (gate_pre / (1.0 + jnp.exp(-gate_pre)) * up_pre).astype(BF16)
    def down(t):
        at = pl.ds(pl.multiple_of(t * cols, cols), cols)
        return dot(act, w_down[0, :, at]).astype(BF16)

    parts = []
    for d in far_first(n_tp):
        to = tp_peer(d)
        e_send[to] = down(to)
        parts.append(go(tp_copy(4, d, e_send.at[to], e_recv.at[tp], to)))
    e_recv[tp] = down(tp)
    for copy in sides:
        copy.wait_recv()
    result = mid_buf[tp]
    for t in range(n_tp):
        result = result + s_recv[t].astype(F32)
    ids = load.expert_ids()[...]
    weights = load.expert_weights()[...]
    for copy in parts:
        copy.wait_recv()
    summed = e_recv[0].astype(F32)
    for t in range(1, n_tp):
        summed = summed + e_recv[t].astype(F32)
    for g in range(n_ep):
        r_send[g] = summed[g * rows : (g + 1) * rows].astype(BF16)
    returns = [
        go(ep_copy(1, d, r_send.at[ep_peer(d)], r_recv.at[ep], ep_peer(d))) for d in far_first(n_ep)
    ]
    r_recv[ep] = r_send[ep]
    for copy in returns:
        copy.wait_recv()
    for e in range(n_ep):
        weight = jnp.sum(jnp.where(ids == e, weights, 0.0), axis=1, keepdims=True)
        result = result + weight * r_recv[e].astype(F32)
    out_ref[...] = result.astype(BF16)
    for copy in started:
        copy.wait_send()


def on_device(
    n_ep,
    n_tp,
    hidden,
    lengths,
    latent_cache,
    cache_rotary,
    attn_gain,
    w_query_nope,
    w_query_rope,
    latent_weight,
    w_rotary_key,
    latent_norm_gain,
    key_up_weight,
    value_up_weight,
    head_gain,
    w_output,
    ffn_gain,
    expert_ids,
    expert_weights,
    w_expert_gate,
    w_expert_up,
    w_expert_down,
    w_shared_gate,
    w_shared_up,
    w_shared_down,
    w_dense_up,
    w_dense_down,
    dense_gate,
):
    arrays = Arrays(
        hidden=hidden,
        attn_gain=attn_gain,
        w_query_nope=w_query_nope,
        w_query_rope=w_query_rope,
        key_up_weight=key_up_weight,
        latent_norm_gain=latent_norm_gain,
        w_rotary_key=w_rotary_key.T,
        latent_weight=latent_weight,
        cache_rotary=cache_rotary.reshape(cache_rotary.shape[1:]),
        latent_cache=latent_cache.reshape(latent_cache.shape[1:]),
        value_up_weight=value_up_weight,
        head_gain=head_gain,
        w_output=w_output,
        ffn_gain=ffn_gain,
        dense_gate=dense_gate,
        expert_ids=expert_ids,
        expert_weights=expert_weights,
        w_shared_gate=w_shared_gate,
        w_shared_up=w_shared_up,
        w_dense_up=w_dense_up,
        w_shared_down=w_shared_down,
        w_dense_down=w_dense_down,
        w_expert_gate=w_expert_gate,
        w_expert_up=w_expert_up,
        w_expert_down=w_expert_down,
    )
    rows, width = hidden.shape
    heads = w_query_nope.shape[1] // PLAIN_QUERY
    latent = latent_cache.shape[2]
    cols = width // n_tp
    message = latent + 128
    any_space = pl.BlockSpec(memory_space=pltpu.HBM)
    return pl.pallas_call(
        functools.partial(layer_kernel, n_ep, n_tp),
        out_shape=pltpu.VMEM((rows, cols), BF16),
        in_specs=[any_space] * (1 + len(arrays)),
        out_specs=pl.BlockSpec(memory_space=pltpu.VMEM),
        scratch_shapes=[VMEM(a.shape, a.dtype) for a in arrays]
        + [
            VMEM(lengths.shape, lengths.dtype),
            pltpu.SemaphoreType.DMA((len(arrays) + 1,)),
            VMEM((rows, heads, message), BF16),
            VMEM((n_tp, heads, message), BF16),
            VMEM((n_tp, heads, latent), BF16),
            VMEM((n_tp, heads, latent), BF16),
            VMEM((n_tp, rows, width), BF16),
            VMEM((n_tp, rows, cols), F32),
            VMEM((n_ep, rows, width), BF16),
            VMEM((n_tp, rows, cols), BF16),
            VMEM((n_tp, rows, cols), BF16),
            VMEM((n_tp, n_ep * rows, cols), BF16),
            VMEM((n_tp, n_ep * rows, cols), BF16),
            VMEM((n_ep, rows, cols), BF16),
            VMEM((n_ep, rows, cols), BF16),
            pltpu.SemaphoreType.DMA((5, 2, n_tp)),
            pltpu.SemaphoreType.DMA((2, 2, n_ep)),
            pltpu.SemaphoreType.REGULAR((meet_rounds(n_ep), 2)),
        ],
        compiler_params=pltpu.CompilerParams(
            collective_id=0, has_side_effects=True, vmem_limit_bytes=60 * 1024 * 1024
        ),
    )(lengths, *arrays)


def solution(mesh):
    placed = (
        P("ep", None),
        P(("ep", "tp")),
        P(("ep", "tp"), None, None),
        P(("ep", "tp"), None, None),
        P(),
        P(None, "tp"),
        P(None, "tp"),
        P(),
        P(),
        P(),
        P("tp", None),
        P(None, "tp"),
        P("tp"),
        P("tp", None),
        P(),
        P("ep", None),
        P("ep", None),
        P("ep", None, "tp"),
        P("ep", None, "tp"),
        P("ep", "tp", None),
        P(None, "tp"),
        P(None, "tp"),
        P("tp", None),
        P(None, "tp"),
        P("tp", None),
        P(),
    )
    step = functools.partial(on_device, mesh.shape["ep"], mesh.shape["tp"])
    return jax.shard_map(
        step, mesh=mesh, in_specs=placed, out_specs=P("ep", "tp"), check_vma=False
    )
```
